256 devices in a mesh: sp: 32 (over z, x), tp: 8 (over y, core).
Axes of the slice: x: 4, y: 4, z: 8, core: 2. Of those that a mesh axis runs over, the one named last changes fastest.
Arguments:
- broad_probe_tensor: bfloat16 [16384, 1024], P('sp', 'tp'), may hold values from -6 to 6
- broad_lookup_tensor: bfloat16 [16384, 1024], P('sp', 'tp'), may hold values from -6 to 6
- broad_payload_tensor: bfloat16 [16384, 1024], P('sp', 'tp'), may hold values from -6 to 6
- broad_emission_valve: bfloat16 [16384, 1024], P('sp', 'tp'), may hold values from -6 to 6
- slim_probe_tensor: bfloat16 [16384, 1024], P('sp', 'tp'), may hold values from -6 to 6
- slim_lookup_tensor: bfloat16 [16384, 1024], P('sp', 'tp'), may hold values from -6 to 6
- slim_payload_tensor: bfloat16 [16384, 1024], P('sp', 'tp'), may hold values from -6 to 6
- slim_emission_valve: bfloat16 [16384, 1024], P('sp', 'tp'), may hold values from -6 to 6
- broad_forgetting_speed: float32 [8], P('tp'), may hold values from -0.08 to 0
- slim_forgetting_speed: float32 [16], P('tp'), may hold values from -0.08 to 0
- broad_channel_scaling: float32 [1024], P('tp'), may hold values from 0.1 to 1.9
- slim_channel_scaling: float32 [1024], P('tp'), may hold values from 0.1 to 1.9
- surge_forgetting: float32 [16384], P('sp'), may hold values from -2.1 to 0
- broad_emission_proj: bfloat16 [1024, 2048], replicated, may hold values from -0.125 to 0.125
- slim_emission_proj: bfloat16 [1024, 2048], replicated, may hold values from -0.125 to 0.125
- skip_stream: bfloat16 [16384, 2048], P(('sp', 'tp')), may hold values from -6 to 6
- premix_scaling_coeffs: float32 [2048], replicated, may hold values from 0.1 to 1.9
- routed_specialist_ids: int32 [16384, 2], P('sp'), may hold values from 0 to 31, as said below
- routed_specialist_shares: float32 [16384, 2], P('sp'), may hold values from 0.2 to 1
- specialist_valve_proj: bfloat16 [32, 2048, 2048], P('sp', None, 'tp'), may hold values from -0.125 to 0.125
- specialist_expand_proj: bfloat16 [32, 2048, 2048], P('sp', None, 'tp'), may hold values from -0.125 to 0.125
- specialist_contract_proj: bfloat16 [32, 2048, 2048], P('sp', 'tp'), may hold values from -0.125 to 0.125
Outputs:
- result: bfloat16 [16384, 2048], P(('sp', 'tp'))
The draws below stay inside these ranges and needn't reach their ends.
Inputs may be any that keep to these rules, and one draw needn't show every extreme that they name: `routed_specialist_ids`: each row names two different experts of one group, that is of the same run of 8 consecutive experts. The rows of one device (each aligned block of 64 rows) name each expert at most 8 times, and some expert is named exactly 8 times by the rows of every device.
All inputs are finite; a program needn't handle non-finite values.
Results may differ from the reference program's by a relative error of at most 0.018.
Values may be sent and summed in bfloat16 or wider, within the bound.
A program may use at most 128 MiB of HBM per device.

```python
import jax
import jax.numpy as jnp
from jax import lax

D = 2048
HA = 8
BROAD_CHANNEL_DIM = 128
HB = 16
THIN_CHANNEL_DIM = 64
FFE = 2048
GROUPS = 4
EXPERTS = 32
EXP_GROUP = 8
ROWS = 64
CAP = 8
TOKENS = 16384
BLOCK = 512
N_SP = 32
N_TP = 8


def rate_law(key, heads):
    pick_key, fast_key, slow_key = jax.random.split(key, 3)
    share = 5
    fast = jax.random.randint(pick_key, (heads,), 0, 10) < share
    span = jax.random.uniform(fast_key, (heads,), jnp.float32, 30.0, 100.0)
    slow = jnp.exp(jax.random.uniform(slow_key, (heads,), jnp.float32, jnp.log(0.02), jnp.log(0.2))) / TOKENS
    return jnp.where(fast, -jnp.log(10.0) / span, -slow).astype(jnp.float32)


def draw_broad_forgetting_speed(key, part):
    return rate_law(jax.random.fold_in(key, 11), HA)


def draw_slim_forgetting_speed(key, part):
    return rate_law(jax.random.fold_in(key, 12), HB)


def draw_surge_forgetting(key, part):
    where_key, size_key = jax.random.split(jax.random.fold_in(key, 21))
    spots = jax.random.randint(where_key, (3,), 0, TOKENS)
    kept = jax.random.uniform(size_key, (3,), jnp.float32, 0.5, 0.8)
    places = jnp.arange(TOKENS, dtype=jnp.int32)
    marks = jnp.where(places[None, :] == spots[:, None], jnp.log(kept)[:, None], 0.0)
    return jnp.sum(marks, 0).astype(jnp.float32)


def draw_routed_specialist_ids(key, part):
    base = jax.random.fold_in(key, 31)
    busy = jax.random.randint(jax.random.fold_in(base, 0), (), 0, GROUPS)
    blocks = TOKENS // ROWS
    units = CAP // 2

    def one(index):
        block_key = jax.random.fold_in(base, index + 1)
        cut_key, perm_key, offset_key, stride_key = jax.random.split(block_key, 4)
        cuts = jnp.sort(jax.random.randint(cut_key, (GROUPS - 2,), 0, units + 1))
        edges = jnp.concatenate([jnp.zeros((1,), jnp.int32), cuts, jnp.full((1,), units, jnp.int32)])
        counts = jnp.concatenate([jnp.full((1,), ROWS // 2, jnp.int32), (edges[1:] - edges[:-1]) * EXP_GROUP])
        ends = jnp.cumsum(counts)
        starts = ends - counts
        slot = jax.random.permutation(perm_key, ROWS)
        order = jnp.sum((slot[:, None] >= ends[None, :]).astype(jnp.int32), 1)
        inside = slot - starts[order]
        group = (busy + order) % GROUPS
        segment_begin = jax.random.randint(offset_key, (GROUPS,), 0, EXP_GROUP)
        stride = jax.random.randint(stride_key, (GROUPS,), 1, EXP_GROUP)
        first = group * EXP_GROUP + (segment_begin[group] + inside) % EXP_GROUP
        second = group * EXP_GROUP + (segment_begin[group] + inside + stride[group]) % EXP_GROUP
        return jnp.stack([first, second], 1)
    return jax.vmap(one)(jnp.arange(blocks, dtype=jnp.int32)).reshape(TOKENS, 2).astype(jnp.int32)


def steps_of(rng, dims, shards, smallest, largest):
    loudness = 1.0
    for position, parts in shards:
        heights = jax.random.uniform(jax.random.fold_in(jax.random.fold_in(rng, 6), position), (parts,), jnp.float32, smallest / len(shards), largest / len(shards))
        loudness = loudness * jnp.repeat(jnp.exp(heights), dims[position] // parts).reshape((-1,) + (1,) * (len(dims) - 1 - position))
    return loudness


def noise(stream_key, dims, scale, limit, cuts=(), kind=jnp.bfloat16):
    loudness = steps_of(stream_key, dims, cuts, -0.22, 0.18) if cuts else 1.0
    entries = jax.random.normal(stream_key, dims, jnp.float32) * scale * loudness
    return jnp.minimum(jnp.maximum(entries, -limit), limit).astype(kind)


def setup_inputs(seed: int = 0) -> dict:
    keys = jax.random.split(jax.random.key(seed), 23)
    return {
        "broad_probe_tensor": noise(keys[0], (TOKENS, HA * BROAD_CHANNEL_DIM), 1.0, 6.0, ((0, 32), (1, 8))),
        "broad_lookup_tensor": noise(keys[1], (TOKENS, HA * BROAD_CHANNEL_DIM), 1.0, 6.0, ((0, 32), (1, 8))),
        "broad_payload_tensor": noise(keys[2], (TOKENS, HA * BROAD_CHANNEL_DIM), 1.0, 6.0, ((0, 32), (1, 8))),
        "broad_emission_valve": noise(keys[3], (TOKENS, HA * BROAD_CHANNEL_DIM), 1.0, 6.0, ((0, 32), (1, 8))),
        "slim_probe_tensor": noise(keys[4], (TOKENS, HB * THIN_CHANNEL_DIM), 1.0, 6.0, ((0, 32), (1, 8))),
        "slim_lookup_tensor": noise(keys[5], (TOKENS, HB * THIN_CHANNEL_DIM), 1.0, 6.0, ((0, 32), (1, 8))),
        "slim_payload_tensor": noise(keys[6], (TOKENS, HB * THIN_CHANNEL_DIM), 1.0, 6.0, ((0, 32), (1, 8))),
        "slim_emission_valve": noise(keys[7], (TOKENS, HB * THIN_CHANNEL_DIM), 1.0, 6.0, ((0, 32), (1, 8))),
        "broad_forgetting_speed": draw_broad_forgetting_speed(jax.random.fold_in(keys[22], 71), 0),
        "slim_forgetting_speed": draw_slim_forgetting_speed(jax.random.fold_in(keys[22], 71), 0),
        "broad_channel_scaling": jnp.clip(1.0 + 0.18 * jax.random.normal(keys[10], (HA * BROAD_CHANNEL_DIM,), jnp.float32), 0.1, 1.9),
        "slim_channel_scaling": jnp.clip(1.0 + 0.18 * jax.random.normal(keys[11], (HB * THIN_CHANNEL_DIM,), jnp.float32), 0.1, 1.9),
        "surge_forgetting": draw_surge_forgetting(jax.random.fold_in(keys[22], 71), 0),
        "broad_emission_proj": noise(keys[13], (HA * BROAD_CHANNEL_DIM, D), (HA * BROAD_CHANNEL_DIM + HB * THIN_CHANNEL_DIM) ** -0.5, 0.125),
        "slim_emission_proj": noise(keys[14], (HB * THIN_CHANNEL_DIM, D), (HA * BROAD_CHANNEL_DIM + HB * THIN_CHANNEL_DIM) ** -0.5, 0.125),
        "skip_stream": noise(keys[15], (TOKENS, D), 1.0, 6.0, ((0, 256),)),
        "premix_scaling_coeffs": jnp.clip(1.0 + 0.18 * jax.random.normal(keys[16], (D,), jnp.float32), 0.1, 1.9),
        "routed_specialist_ids": draw_routed_specialist_ids(jax.random.fold_in(keys[22], 71), 0),
        "routed_specialist_shares": jnp.clip(0.2 + 0.8 * jax.random.uniform(keys[18], (TOKENS, 2), jnp.float32) ** steps_of(keys[18], (TOKENS, 2), ((0, 32),), -0.2, 0.2), 0.2, 1.0),
        "specialist_valve_proj": noise(keys[19], (EXPERTS, D, FFE), D ** -0.5, 0.125, ((0, 32), (2, 8))),
        "specialist_expand_proj": noise(keys[20], (EXPERTS, D, FFE), D ** -0.5, 0.125, ((0, 32), (2, 8))),
        "specialist_contract_proj": noise(keys[21], (EXPERTS, FFE, D), FFE ** -0.5, 0.125, ((0, 32), (1, 8))),
    }


rope_base = 10000.0
epsilon = 1e-06

def rotate(payload_tensor, positions):
    channel_dimension = payload_tensor.shape[-1]
    half = channel_dimension // 2
    freq = rope_base ** (-jnp.arange(half, dtype=jnp.float32) * 2.0 / channel_dimension)
    angle = positions.astype(jnp.float32)[:, None, None] * freq[None, None, :]
    cosine = jnp.cos(angle)
    sine = jnp.sin(angle)
    first = payload_tensor[..., :half]
    second = payload_tensor[..., half:]
    return jnp.concatenate([first * cosine - second * sine, first * sine + second * cosine], -1)

def prepare(probe_source, lookup_tensor, payload_tensor, heads, channel_dimension):
    length = probe_source.shape[0]
    places = jnp.arange(length, dtype=jnp.int32)
    spun_probe = rotate(probe_source.astype(jnp.float32).reshape(length, heads, channel_dimension), places).astype(jnp.bfloat16)
    spun_lookup = (rotate(lookup_tensor.astype(jnp.float32).reshape(length, heads, channel_dimension), places) * channel_dimension ** (-0.5)).astype(jnp.bfloat16)
    return (spun_probe, spun_lookup, payload_tensor.reshape(length, heads, channel_dimension))

def segment_terms(probe_tensor, lookup_tensor, payload_tensor, surge_forgetting, forgetting_speed):
    length = probe_tensor.shape[0]
    segment_tally = jnp.arange(length, dtype=jnp.float32)
    memory_matrix = forgetting_speed[None, :] * segment_tally[:, None] + jnp.cumsum(surge_forgetting)[:, None]
    causal = (segment_tally[:, None] >= segment_tally[None, :])[None]
    level_t = jnp.transpose(memory_matrix)
    gap = level_t[:, :, None] - level_t[:, None, :]
    decay = jnp.where(causal, jnp.exp(jnp.where(causal, gap, 0.0)), 0.0)
    attention_scores = jnp.einsum('szr,yzr->zsy', probe_tensor.astype(jnp.float32), lookup_tensor.astype(jnp.float32))
    weights = (attention_scores * decay).astype(jnp.bfloat16)
    inner = jnp.einsum('htm,mhe->the', weights.astype(jnp.float32), payload_tensor.astype(jnp.float32))
    factor = jnp.exp(memory_matrix + forgetting_speed[None, :])
    tail = jnp.exp(memory_matrix[-1:, :] - memory_matrix)
    weighted_output = (lookup_tensor.astype(jnp.float32) * tail[:, :, None]).astype(jnp.bfloat16)
    state_update = jnp.einsum('oup,our->upr', weighted_output.astype(jnp.float32), payload_tensor.astype(jnp.float32))
    total = jnp.exp(memory_matrix[-1] + forgetting_speed)
    return (inner, factor, state_update, total)

def read_state(probe_tensor, state):
    return jnp.einsum('thd,hde->the', probe_tensor.astype(jnp.float32), state, precision=lax.Precision.HIGHEST)

def finish(sublayer_final, emission_valve, scaling_coefficients):
    length, heads, channel_dimension = sublayer_final.shape
    normed = sublayer_final * lax.rsqrt(lax.optimization_barrier(jnp.mean(sublayer_final * sublayer_final, -1, keepdims=True)) + epsilon)
    gated = normed.reshape(length, heads * channel_dimension) * scaling_coefficients[None, :] * jax.nn.silu(emission_valve.astype(jnp.float32))
    return gated.astype(jnp.bfloat16)

def keeping_multiplier(probe_source, lookup_tensor, payload_tensor, emission_valve, forgetting_speed, scaling_coefficients, surge_forgetting, channel_dimension):
    heads = probe_source.shape[1] // channel_dimension
    spun_probe, spun_lookup, regrouped_payload = prepare(probe_source, lookup_tensor, payload_tensor, heads, channel_dimension)
    count = TOKENS // BLOCK

    def divider_mark(array):
        return array.reshape((count, BLOCK) + array.shape[1:])

    def segment_walker(state, piece):
        block_q, block_k, block_v, block_b = piece
        inner, factor, state_update, total = segment_terms(block_q, block_k, block_v, block_b, forgetting_speed)
        sublayer_final = inner + factor[:, :, None] * read_state(block_q, state)
        return (total[:, None, None] * state + state_update, sublayer_final)
    opening_location = jnp.zeros((heads, channel_dimension, channel_dimension), jnp.float32)
    ignored_placeholder, sublayer_final = lax.scan(segment_walker, opening_location, (divider_mark(spun_probe), divider_mark(spun_lookup), divider_mark(regrouped_payload), divider_mark(surge_forgetting)))
    return finish(sublayer_final.reshape(TOKENS, heads, channel_dimension), emission_valve, scaling_coefficients)

def experts_mix(normed, routed_specialist_ids, routed_specialist_shares, specialist_valve_proj, specialist_expand_proj, specialist_contract_proj):
    most = N_SP * N_TP * CAP
    slice_width = FFE // N_TP
    padded = jnp.concatenate([normed, jnp.zeros((1, D), jnp.bfloat16)], 0)

    def one(accum, index):
        matches = routed_specialist_ids == index
        weight = lax.optimization_barrier(jnp.sum(jnp.where(matches, routed_specialist_shares, 0.0), 1))
        weight = jnp.concatenate([weight, jnp.zeros((1,), jnp.float32)], 0)
        picked = jnp.nonzero(jnp.any(matches, 1), size=most, fill_value=TOKENS)[0].astype(jnp.int32)
        taken = padded[picked]
        emission_valve = jnp.dot(taken, specialist_valve_proj[index], preferred_element_type=jnp.float32)
        up = jnp.dot(taken, specialist_expand_proj[index], preferred_element_type=jnp.float32)
        hidden = (jax.nn.silu(emission_valve) * up).astype(jnp.bfloat16).reshape(most, N_TP, slice_width)
        down = specialist_contract_proj[index].reshape(N_TP, slice_width, D)
        partial_value = jnp.einsum('mpf,pfd->pmd', hidden.astype(jnp.float32), down.astype(jnp.float32))
        rounded = lax.optimization_barrier(partial_value.astype(jnp.bfloat16))
        expert_out = lax.optimization_barrier(jnp.sum(rounded.astype(jnp.float32), 0)).astype(jnp.bfloat16)
        accum = accum.at[picked].add(weight[picked][:, None] * expert_out.astype(jnp.float32))
        return (accum, None)
    opening_location = jnp.zeros((TOKENS + 1, D), jnp.float32)
    accum, ignored_placeholder = lax.scan(one, opening_location, jnp.arange(EXPERTS, dtype=jnp.int32))
    return accum[:TOKENS]

def reference(broad_probe_tensor, broad_lookup_tensor, broad_payload_tensor, broad_emission_valve, slim_probe_tensor, slim_lookup_tensor, slim_payload_tensor, slim_emission_valve, broad_forgetting_speed, slim_forgetting_speed, broad_channel_scaling, slim_channel_scaling, surge_forgetting, broad_emission_proj, slim_emission_proj, skip_stream, premix_scaling_coeffs, routed_specialist_ids, routed_specialist_shares, specialist_valve_proj, specialist_expand_proj, specialist_contract_proj):
    broad_channel_total = keeping_multiplier(broad_probe_tensor, broad_lookup_tensor, broad_payload_tensor, broad_emission_valve, broad_forgetting_speed, broad_channel_scaling, surge_forgetting, BROAD_CHANNEL_DIM)
    slim_channel_total = keeping_multiplier(slim_probe_tensor, slim_lookup_tensor, slim_payload_tensor, slim_emission_valve, slim_forgetting_speed, slim_channel_scaling, surge_forgetting, THIN_CHANNEL_DIM)
    projected = jnp.dot(broad_channel_total, broad_emission_proj, preferred_element_type=jnp.float32)
    projected = projected + jnp.dot(slim_channel_total, slim_emission_proj, preferred_element_type=jnp.float32)
    updated = skip_stream.astype(jnp.float32) + projected
    scale = lax.rsqrt(lax.optimization_barrier(jnp.mean(updated * updated, -1, keepdims=True)) + epsilon)
    normed = (updated * scale * premix_scaling_coeffs[None, :]).astype(jnp.bfloat16)
    mixture = experts_mix(normed, routed_specialist_ids, routed_specialist_shares, specialist_valve_proj, specialist_expand_proj, specialist_contract_proj)
    return (updated + mixture).astype(jnp.bfloat16)
```

```python
import jax
import jax.numpy as jnp
from jax import lax
from jax.sharding import Mesh
from jax.sharding import PartitionSpec as P

BROAD_CHANNEL_DIM = 128
THIN_CHANNEL_DIM = 64
GROUPS = 4
SP = ("sp_0", "sp_1")
SP_TP = ("sp_0", "sp_1", "tp")


rope_base = 10000.0
epsilon = 1e-06


def nothing_yet(value, identity):
    return jax.tree.map(
        lambda part, zero: jnp.zeros_like(part) + jnp.asarray(zero, part.dtype), value, identity
    )


def collected_together(value, axis):
    leaves = jax.tree.leaves(value)
    sequence = sorted(range(len(leaves)), key=lambda k: -leaves[k].size)
    width = (1, *leaves[sequence[0]].shape)[-1]
    lines = [
        jnp.pad(leaves[k].reshape(-1), (0, -leaves[k].size % width)).reshape(-1, width)
        for k in sequence
    ]
    both, at, found = (lax.all_gather(jnp.concatenate(lines), axis), 0, {})
    for k, line in zip(sequence, lines):
        slab = both[:, at : at + len(line)].reshape(len(both), -1)
        found[k] = slab[:, : leaves[k].size].reshape(-1, *leaves[k].shape)
        at += len(line)
    numbers = iter(range(len(leaves)))
    return jax.tree.map(lambda _: found[next(numbers)], value)


def prefix_by_axis(value, axes, combine, identity):
    before = start = nothing_yet(value, identity)
    total = value
    for axis in reversed(axes):
        count, here = (lax.axis_size(axis), lax.axis_index(axis))
        pieces = collected_together(
            jax.tree.map(
                lambda part, kind: part.astype(kind),
                total,
                (jnp.bfloat16, jnp.bfloat16, jnp.bfloat16, jnp.bfloat16),
            ),
            axis,
        )
        inside, total = (start, start)
        for k in range(count):
            passed = k < here
            total = combine(
                total, jax.tree.map(lambda part, own: part[k].astype(own.dtype), pieces, value)
            )
            inside = jax.tree.map(lambda new, old: jnp.where(passed, new, old), total, inside)
        before = combine(inside, before)
    return before


def rotate(payload_tensor, positions):
    channel_dimension = payload_tensor.shape[-1]
    half = channel_dimension // 2
    freq = rope_base ** (-jnp.arange(half, dtype=jnp.float32) * 2.0 / channel_dimension)
    angle = positions.astype(jnp.float32)[:, None, None] * freq[None, None, :]
    cosine = jnp.cos(angle)
    sine = jnp.sin(angle)
    first = payload_tensor[..., :half]
    second = payload_tensor[..., half:]
    return jnp.concatenate([first * cosine - second * sine, first * sine + second * cosine], -1)


def segment_terms(probe_tensor, lookup_tensor, payload_tensor, surge_forgetting, forgetting_speed):
    length = probe_tensor.shape[0]
    segment_tally = jnp.arange(length, dtype=jnp.float32)
    memory_matrix = (
        forgetting_speed[None, :] * segment_tally[:, None] + jnp.cumsum(surge_forgetting)[:, None]
    )
    causal = (segment_tally[:, None] >= segment_tally[None, :])[None]
    level_t = jnp.transpose(memory_matrix)
    gap = level_t[:, :, None] - level_t[:, None, :]
    decay = jnp.where(causal, jnp.exp(jnp.where(causal, gap, 0.0)), 0.0)
    attention_scores = jnp.einsum(
        "szr,yzr->zsy", probe_tensor, lookup_tensor, preferred_element_type=jnp.float32
    )
    weights = (attention_scores * decay).astype(jnp.bfloat16)
    inner = jnp.einsum("htm,mhe->the", weights, payload_tensor, preferred_element_type=jnp.float32)
    factor = jnp.exp(memory_matrix + forgetting_speed[None, :])
    tail = jnp.exp(memory_matrix[-1:, :] - memory_matrix)
    weighted_output = (lookup_tensor.astype(jnp.float32) * tail[:, :, None]).astype(jnp.bfloat16)
    state_update = jnp.einsum(
        "oup,our->upr", weighted_output, payload_tensor, preferred_element_type=jnp.float32
    )
    total = jnp.exp(memory_matrix[-1] + forgetting_speed)
    return (inner, factor, state_update, total)


def read_state(probe_tensor, state):
    return jnp.einsum("thd,hde->the", probe_tensor.astype(jnp.float32), state)


def keeping_multiplier(
    probe_source,
    lookup_tensor,
    payload_tensor,
    forgetting_speed,
    surge_forgetting,
    channel_dimension,
    segment_begin,
):
    length = probe_source.shape[0]
    heads = probe_source.shape[1] // channel_dimension
    places = segment_begin + jnp.arange(length, dtype=jnp.int32)
    spun_probe = rotate(
        probe_source.astype(jnp.float32).reshape(length, heads, channel_dimension), places
    ).astype(jnp.bfloat16)
    spun_lookup = (
        rotate(lookup_tensor.astype(jnp.float32).reshape(length, heads, channel_dimension), places)
        * channel_dimension ** (-0.5)
    ).astype(jnp.bfloat16)
    regrouped_payload = payload_tensor.reshape(length, heads, channel_dimension)
    block = min(512, length)
    count = length // block

    def divider_mark(array):
        return array.reshape((count, block) + array.shape[1:])

    def segment_walker(carry, piece):
        state, prefix = carry
        block_q, block_k, block_v, block_b = piece
        inner, factor, state_update, total = segment_terms(
            block_q, block_k, block_v, block_b, forgetting_speed
        )
        local = inner + factor[:, :, None] * read_state(block_q, state)
        return (
            (total[:, None, None] * state + state_update, prefix * total),
            (local, factor * prefix[None, :]),
        )

    opening_location = (
        jnp.zeros((heads, channel_dimension, channel_dimension), jnp.float32),
        jnp.ones((heads,), jnp.float32),
    )
    (state, decay), (local, reach) = lax.scan(
        segment_walker,
        opening_location,
        (
            divider_mark(spun_probe),
            divider_mark(spun_lookup),
            divider_mark(regrouped_payload),
            divider_mark(surge_forgetting),
        ),
    )
    return (
        spun_probe,
        local.reshape(length, heads, channel_dimension),
        reach.reshape(length, heads),
        decay,
        state,
    )


def finish(sublayer_final, emission_valve, scaling_coefficients):
    length, heads, channel_dimension = sublayer_final.shape
    normed = sublayer_final * lax.rsqrt(
        jnp.mean(sublayer_final * sublayer_final, -1, keepdims=True) + epsilon
    )
    gated = (
        normed.reshape(length, heads * channel_dimension)
        * scaling_coefficients[None, :]
        * jax.nn.silu(emission_valve.astype(jnp.float32))
    )
    return gated.astype(jnp.bfloat16)


def chain(earlier, later):
    return (
        earlier[0] * later[0],
        later[0][:, None, None] * earlier[1] + later[1],
        earlier[2] * later[2],
        later[2][:, None, None] * earlier[3] + later[3],
    )


def slot_positions(chosen, experts, cap):
    listed = chosen.reshape(-1)
    matches = (listed[:, None] == jnp.arange(experts, dtype=jnp.int32)[None, :]).astype(jnp.int32)
    before = jnp.cumsum(matches, 0) - matches
    order = jnp.sum(before * matches, 1)
    return (listed * cap + order).reshape(chosen.shape)


def fill_slots(rows_in, chosen, experts, cap):
    count = rows_in.shape[0]
    places = slot_positions(chosen, experts, cap).reshape(-1)
    owners = jnp.repeat(jnp.arange(count, dtype=jnp.int32), 2)
    source = jnp.full((experts * cap,), count, jnp.int32).at[places].set(owners)
    padded = jnp.concatenate([rows_in, jnp.zeros((1, rows_in.shape[1]), rows_in.dtype)], 0)
    return padded[source].reshape(experts, cap, rows_in.shape[1])


def on_device(
    broad_probe_tensor,
    broad_lookup_tensor,
    broad_payload_tensor,
    broad_emission_valve,
    slim_probe_tensor,
    slim_lookup_tensor,
    slim_payload_tensor,
    slim_emission_valve,
    broad_forgetting_speed,
    slim_forgetting_speed,
    broad_channel_scaling,
    slim_channel_scaling,
    surge_forgetting,
    broad_emission_proj,
    slim_emission_proj,
    skip_stream,
    premix_scaling_coeffs,
    routed_specialist_ids,
    routed_specialist_shares,
    specialist_valve_proj,
    specialist_expand_proj,
    specialist_contract_proj,
):
    length = broad_probe_tensor.shape[0]
    segment_begin = lax.axis_index(SP) * length
    valve_all = lax.all_gather(specialist_valve_proj[0], "tp")
    expand_all = lax.all_gather(specialist_expand_proj[0], "tp")
    contract_all = lax.all_gather(specialist_contract_proj[0], "tp")
    wide_result = keeping_multiplier(
        broad_probe_tensor,
        broad_lookup_tensor,
        broad_payload_tensor,
        broad_forgetting_speed,
        surge_forgetting,
        BROAD_CHANNEL_DIM,
        segment_begin,
    )
    narrow_result = keeping_multiplier(
        slim_probe_tensor,
        slim_lookup_tensor,
        slim_payload_tensor,
        slim_forgetting_speed,
        surge_forgetting,
        THIN_CHANNEL_DIM,
        segment_begin,
    )
    identity = (
        jnp.ones_like(wide_result[3]),
        jnp.zeros_like(wide_result[4]),
        jnp.ones_like(narrow_result[3]),
        jnp.zeros_like(narrow_result[4]),
    )
    incoming = prefix_by_axis(
        (wide_result[3], wide_result[4], narrow_result[3], narrow_result[4]), SP, chain, identity
    )
    mixed_wide = finish(
        wide_result[1] + wide_result[2][:, :, None] * read_state(wide_result[0], incoming[1]),
        broad_emission_valve,
        broad_channel_scaling,
    )
    mixed_narrow = finish(
        narrow_result[1] + narrow_result[2][:, :, None] * read_state(narrow_result[0], incoming[3]),
        slim_emission_valve,
        slim_channel_scaling,
    )
    rows_wide, rows_narrow = (
        lax.all_to_all(mixed_wide, "tp", split_axis=0, concat_axis=1, tiled=True),
        lax.all_to_all(mixed_narrow, "tp", split_axis=0, concat_axis=1, tiled=True),
    )
    projected = jnp.dot(rows_wide, broad_emission_proj, preferred_element_type=jnp.float32)
    projected = projected + jnp.dot(
        rows_narrow, slim_emission_proj, preferred_element_type=jnp.float32
    )
    updated = skip_stream.astype(jnp.float32) + projected
    scale = lax.rsqrt(jnp.mean(updated * updated, -1, keepdims=True) + epsilon)
    normed = (updated * scale * premix_scaling_coeffs[None, :]).astype(jnp.bfloat16)
    rows = normed.shape[0]
    width = normed.shape[1]
    experts = lax.axis_size(SP) * specialist_valve_proj.shape[0]
    cap = rows * GROUPS // experts
    own_ids = lax.dynamic_slice_in_dim(routed_specialist_ids, lax.axis_index("tp") * rows, rows, 0)
    own_weights = lax.dynamic_slice_in_dim(
        routed_specialist_shares, lax.axis_index("tp") * rows, rows, 0
    )
    own_places = slot_positions(own_ids, experts, cap)
    sent = lax.all_to_all(
        fill_slots(normed, own_ids, experts, cap), SP, split_axis=0, concat_axis=0, tiled=True
    )
    slots = sent.reshape(-1, width)
    emission_valve = jnp.einsum("sd,tdf->stf", slots, valve_all, preferred_element_type=jnp.float32)
    up = jnp.einsum("sd,tdf->stf", slots, expand_all, preferred_element_type=jnp.float32)
    hidden = (jax.nn.silu(emission_valve) * up).astype(jnp.bfloat16).reshape(slots.shape[0], -1)
    summed = jnp.dot(
        hidden, contract_all.reshape(-1, width), preferred_element_type=jnp.float32
    ).astype(jnp.bfloat16)
    expert_out = summed.reshape(experts, cap, width)
    returned = lax.all_to_all(expert_out, SP, split_axis=0, concat_axis=0, tiled=True)
    picked = returned.reshape(experts * cap, width)[own_places]
    mixture = jnp.sum(own_weights[:, :, None] * picked.astype(jnp.float32), 1)
    return (updated + mixture).astype(jnp.bfloat16)


def solution(mesh):
    finer = Mesh(mesh.devices.reshape(8, 4, mesh.shape["tp"]), ("sp_0", "sp_1", "tp"))
    return jax.shard_map(
        on_device,
        mesh=finer,
        in_specs=(
            P(SP, "tp"),
            P(SP, "tp"),
            P(SP, "tp"),
            P(SP, "tp"),
            P(SP, "tp"),
            P(SP, "tp"),
            P(SP, "tp"),
            P(SP, "tp"),
            P("tp"),
            P("tp"),
            P("tp"),
            P("tp"),
            P(SP),
            P(),
            P(),
            P(SP_TP, None),
            P(),
            P(SP, None),
            P(SP, None),
            P(SP, None, "tp"),
            P(SP, None, "tp"),
            P(SP, "tp", None),
        ),
        out_specs=P(SP_TP, None),
        check_vma=False,
    )
```
